512 devices in a mesh: sp: 64 (over z, y), tp: 8 (over x, core).
Axes of the slice: x: 4, y: 4, z: 16, core: 2. Of those that a mesh axis runs over, the one named last changes fastest.
Arguments:
- tokens: bfloat16 [16384, 2048], P('sp'), may hold values from -6 to 6
- input_norm_gain: float32 [2048], replicated, may hold values from 0.1 to 1.9
- query_matrix: bfloat16 [2048, 1024], P('sp', 'tp'), may hold values from -0.125 to 0.125
- key_matrix: bfloat16 [2048, 1024], P('sp', 'tp'), may hold values from -0.125 to 0.125
- value_matrix: bfloat16 [2048, 1024], P('sp', 'tp'), may hold values from -0.125 to 0.125
- convolution_value_matrix: bfloat16 [2048, 2048], P('sp', 'tp'), may hold values from -0.125 to 0.125
- convolution_gate_matrix: bfloat16 [2048, 2048], P('sp', 'tp'), may hold values from -0.125 to 0.125
- decay_offset_channel: float32 [1024], P('tp'), may hold values from -16 to -2
- decay_first_matrix: bfloat16 [2048, 128], replicated, may hold values from -0.125 to 0.125
- decay_second_matrix: bfloat16 [128, 1024], P(None, 'tp'), may hold values from -0.59765625 to 0.59765625
- learning_rate_offset: float32 [1024], P('tp'), may hold values from -9 to 1
- learning_rate_first_matrix: bfloat16 [2048, 128], replicated, may hold values from -0.125 to 0.125
- learning_rate_second_matrix: bfloat16 [128, 1024], P(None, 'tp'), may hold values from -0.5 to 0.5
- forgetting_rate_factor: float32 [16384, 16], P('sp', 'tp'), may hold values from 0.39 to 2.53
- state_retention_share: float32 [16384, 16], P('sp', 'tp'), may hold values from 0.12 to 1
- per_head_norm_gain: float32 [1024], P('tp'), may hold values from 0.1 to 1.9
- convolution_filter_taps: float32 [31, 2048], P(None, 'tp'), may hold values from -81 to 81
- convolution_channel_gain: float32 [2048], P('tp'), may hold values from 0.1 to 1.9
- attention_output_matrix: bfloat16 [2048, 1024], P('sp', 'tp'), may hold values from -0.109375 to 0.109375
- convolution_output_matrix: bfloat16 [2048, 2048], P('sp', 'tp'), may hold values from -0.109375 to 0.109375
Outputs:
- mixed: bfloat16 [16384, 2048], P('sp')
The draws below stay inside these ranges and needn't reach their ends.
All inputs are finite; a program needn't handle non-finite values.
Results may differ from the reference program's by a relative error of at most 0.014.
Values may be sent and summed in bfloat16 or wider, within the bound.
No kernel may reach another device: no remote copies, remote signals or barrier semaphores. Data moves between devices by JAX's collectives and lax.ppermute only.
A program may use at most 64 MiB of HBM per device.

```python
import jax
import jax.numpy as jnp
from jax import lax

D = 2048
RHEADS = 16
HEAD = 64
RW = 1024
CONV_CH = 2048
CONV_SPAN = 31
LOWRANK = 128
TOK_DEV = 256
TOKENS = 16384
N_TP = 8


def rate_levels(key):
    order = jax.random.permutation(jax.random.fold_in(key, 11), RHEADS)
    fast_count = RHEADS // 2
    fast = jnp.repeat(order < fast_count, HEAD)
    spread = jax.random.uniform(jax.random.fold_in(key, 12), (RW,), jnp.float32)
    other = jax.random.uniform(jax.random.fold_in(key, 13), (RW,), jnp.float32)
    fast_log = jnp.log(1.0 / 60.0) + spread * jnp.log(3.0)
    slow_log = jnp.log(0.01 / TOKENS) + spread * jnp.log(5.0)
    decay_level = jnp.where(fast, fast_log, slow_log) + 0.5
    rate_level = jnp.where(fast, 2.0 * other - 1.0, jnp.log(10.0 / TOKENS) + other - 0.5)
    return (decay_level, rate_level)


def draw_decay_offset_channel(key, part):
    return rate_levels(key)[0]


def draw_learning_rate_offset(key, part):
    return rate_levels(key)[1]


def draw_forgetting_rate_factor(key, part):
    spans = TOKENS // TOK_DEV
    level = jnp.exp(jax.random.uniform(jax.random.fold_in(key, 21), (spans, RHEADS), jnp.float32, -0.7, 0.7))
    rough = jax.random.uniform(jax.random.fold_in(key, 22), (TOKENS, RHEADS), jnp.float32, 0.8, 1.25)
    return jnp.repeat(level, TOK_DEV, axis=0) * rough


def draw_state_retention_share(key, part):
    places = jax.random.randint(jax.random.fold_in(key, 31), (3, RHEADS), 0, TOKENS)
    depth = jax.random.uniform(jax.random.fold_in(key, 32), (3, RHEADS), jnp.float32, 0.6, 0.8)
    struck = jnp.arange(TOKENS, dtype=jnp.int32)[:, None, None] == places[None]
    return jnp.prod(jnp.where(struck, depth[None], 1.0), axis=1)


def draw_convolution_filter_taps(key, part):
    taps = jnp.exp(jax.random.uniform(jax.random.fold_in(key, 41), (CONV_SPAN, 1), jnp.float32, 0.0, jnp.log(10.0)))
    place = jnp.arange(CONV_CH, dtype=jnp.float32)[None, :] / CONV_CH
    rising = jnp.exp(place * jnp.log(10.0))
    rough = jax.random.uniform(jax.random.fold_in(key, 42), (1, CONV_CH), jnp.float32, 0.5, 1.5)
    base = jax.random.truncated_normal(jax.random.fold_in(key, 43), -4.0, 4.0, (CONV_SPAN, CONV_CH), jnp.float32)
    return base * taps * rising * rough / (4.0 * CONV_SPAN ** 0.5)


def block_scale(key, dims, shards, smallest, largest):
    def one(dim, blocks):
        draws = jax.random.uniform(jax.random.fold_in(jax.random.fold_in(key, 6), dim), (blocks,), jnp.float32, smallest / len(shards), largest / len(shards))
        return jnp.repeat(jnp.exp(draws), dims[dim] // blocks).reshape((-1,) + (1,) * (len(dims) - dim - 1))

    loudness = one(*shards[0])
    for cut in shards[1:]:
        loudness = loudness * one(*cut)
    return loudness


def bell_draw(stream_key, extent, width, bound, split=(), kind=jnp.bfloat16):
    entries = jax.random.normal(stream_key, extent, jnp.float32) * width
    if len(split) > 0:
        entries = block_scale(stream_key, extent, split, -0.22, 0.18) * entries
    return jnp.clip(entries, min=-bound, max=bound).astype(kind)


def setup_inputs(seed: int = 0) -> dict:
    arg_keys = jax.random.split(jax.random.key(seed), 21)
    return {
        "tokens": bell_draw(arg_keys[0], (TOKENS, D), 1.0, 6.0, ((0, 64),)),
        "input_norm_gain": jnp.clip(1.0 + 0.18 * jax.random.normal(arg_keys[1], (D,), jnp.float32), 0.1, 1.9),
        "query_matrix": bell_draw(arg_keys[2], (D, RW), D ** -0.5, 0.125, ((0, 64), (1, 8))),
        "key_matrix": bell_draw(arg_keys[3], (D, RW), D ** -0.5, 0.125, ((0, 64), (1, 8))),
        "value_matrix": bell_draw(arg_keys[4], (D, RW), D ** -0.5, 0.125, ((0, 64), (1, 8))),
        "convolution_value_matrix": bell_draw(arg_keys[5], (D, CONV_CH), D ** -0.5, 0.125, ((0, 64), (1, 8))),
        "convolution_gate_matrix": bell_draw(arg_keys[6], (D, CONV_CH), D ** -0.5, 0.125, ((0, 64), (1, 8))),
        "decay_offset_channel": draw_decay_offset_channel(jax.random.fold_in(arg_keys[20], 71), 0),
        "decay_first_matrix": bell_draw(arg_keys[8], (D, LOWRANK), D ** -0.5, 0.125),
        "decay_second_matrix": bell_draw(arg_keys[9], (LOWRANK, RW), 0.1, 0.59765625, ((1, 8),)),
        "learning_rate_offset": draw_learning_rate_offset(jax.random.fold_in(arg_keys[20], 71), 0),
        "learning_rate_first_matrix": bell_draw(arg_keys[11], (D, LOWRANK), D ** -0.5, 0.125),
        "learning_rate_second_matrix": bell_draw(arg_keys[12], (LOWRANK, RW), LOWRANK ** -0.5, 0.5, ((1, 8),)),
        "forgetting_rate_factor": draw_forgetting_rate_factor(jax.random.fold_in(arg_keys[20], 71), 0),
        "state_retention_share": draw_state_retention_share(jax.random.fold_in(arg_keys[20], 71), 0),
        "per_head_norm_gain": jnp.clip(1.0 + 0.18 * jax.random.normal(arg_keys[15], (RW,), jnp.float32), 0.1, 1.9),
        "convolution_filter_taps": draw_convolution_filter_taps(jax.random.fold_in(arg_keys[20], 71), 0),
        "convolution_channel_gain": jnp.clip(1.0 + 0.18 * jax.random.normal(arg_keys[17], (CONV_CH,), jnp.float32), 0.1, 1.9),
        "attention_output_matrix": bell_draw(arg_keys[18], (D, RW), (RW + CONV_CH) ** -0.5, 0.109375, ((0, 64), (1, 8))),
        "convolution_output_matrix": bell_draw(arg_keys[19], (D, CONV_CH), (RW + CONV_CH) ** -0.5, 0.109375, ((0, 64), (1, 8))),
    }


HIGHEST = lax.Precision.HIGHEST

def reference(tokens, input_norm_gain, query_matrix, key_matrix, value_matrix, convolution_value_matrix, convolution_gate_matrix, decay_offset_channel, decay_first_matrix, decay_second_matrix, learning_rate_offset, learning_rate_first_matrix, learning_rate_second_matrix, forgetting_rate_factor, state_retention_share, per_head_norm_gain, convolution_filter_taps, convolution_channel_gain, attention_output_matrix, convolution_output_matrix):
    widened = tokens.astype(jnp.float32)
    normed = (widened * lax.rsqrt(lax.optimization_barrier(jnp.mean(widened * widened, axis=-1, keepdims=True)) + 1e-06) * input_norm_gain).astype(jnp.bfloat16)
    query_proj = jnp.dot(normed, query_matrix, preferred_element_type=jnp.float32)
    key_proj = jnp.dot(normed, key_matrix, preferred_element_type=jnp.float32)
    value_proj = jnp.dot(normed, value_matrix, preferred_element_type=jnp.float32)
    conv_value = jnp.dot(normed, convolution_value_matrix, preferred_element_type=jnp.float32)
    conv_gate = jnp.dot(normed, convolution_gate_matrix, preferred_element_type=jnp.float32)
    decay_mid = jnp.tanh(jnp.dot(normed, decay_first_matrix, preferred_element_type=jnp.float32)).astype(jnp.bfloat16)
    rate_mid = jnp.dot(normed, learning_rate_first_matrix, preferred_element_type=jnp.float32).astype(jnp.bfloat16)
    logarithm_learning_rate = -jax.nn.softplus(-(decay_offset_channel + jnp.dot(decay_mid, decay_second_matrix, preferred_element_type=jnp.float32))) - 0.5
    learn_rate = jax.nn.sigmoid(learning_rate_offset + jnp.dot(rate_mid, learning_rate_second_matrix, preferred_element_type=jnp.float32))
    reshaped_tensor = (TOKENS, RHEADS, HEAD)
    position_decay_factor = jnp.exp(-jnp.exp(logarithm_learning_rate).reshape(reshaped_tensor) * forgetting_rate_factor[:, :, None]) * state_retention_share[:, :, None]
    key_heads = key_proj.reshape(reshaped_tensor)
    unit_key = key_heads * lax.rsqrt(lax.optimization_barrier(jnp.sum(key_heads * key_heads, axis=-1, keepdims=True)) + 1e-06)
    erase = -unit_key
    write = unit_key * learn_rate.reshape(reshaped_tensor)

    def advance(state, inputs):
        query_t, decay_t, key_t, value_t, erase_t, write_t = inputs
        pulled = jnp.einsum('hvk,hk->hv', state, erase_t, precision=HIGHEST)
        state = state * decay_t[:, None, :] + pulled[:, :, None] * write_t[:, None, :] + value_t[:, :, None] * key_t[:, None, :]
        return (state, jnp.einsum('hvk,hk->hv', state, query_t, precision=HIGHEST))
    final_state, state_rows = lax.scan(advance, jnp.zeros((RHEADS, HEAD, HEAD), jnp.float32), (query_proj.reshape(reshaped_tensor), position_decay_factor, key_heads, value_proj.reshape(reshaped_tensor), erase, write))
    centred = state_rows - lax.optimization_barrier(jnp.mean(state_rows, axis=-1, keepdims=True))
    normal_state = centred * lax.rsqrt(lax.optimization_barrier(jnp.mean(centred * centred, axis=-1, keepdims=True)) + 0.00064)
    state_mixed = (normal_state * per_head_norm_gain.reshape(RHEADS, HEAD)).reshape(TOKENS, RW).astype(jnp.bfloat16)
    gated = (conv_value * jax.nn.sigmoid(conv_gate)).astype(jnp.bfloat16)
    padded = jnp.concatenate([jnp.zeros((CONV_SPAN - 1, CONV_CH), jnp.bfloat16), gated], axis=0)
    filtered = jnp.zeros((TOKENS, CONV_CH), jnp.float32)
    for offset in range(CONV_SPAN):
        filtered = filtered + convolution_filter_taps[offset] * padded[offset:offset + TOKENS].astype(jnp.float32)
    row_mean = lax.optimization_barrier(jnp.mean(filtered, axis=-1, keepdims=True))
    deviation = filtered - row_mean
    variance = lax.optimization_barrier(jnp.mean(deviation * deviation, axis=-1, keepdims=True))
    conv_mixed = jax.nn.silu(deviation * lax.rsqrt(variance + 1e-05) * convolution_channel_gain).astype(jnp.bfloat16)
    state_part = RW // N_TP
    conv_part = CONV_CH // N_TP
    total = jnp.zeros((TOKENS, D), jnp.float32)
    for member in range(N_TP):
        state_lo = member * state_part
        conv_lo = member * conv_part
        partial_value = jnp.dot(state_mixed[:, state_lo:state_lo + state_part], attention_output_matrix[:, state_lo:state_lo + state_part].T, preferred_element_type=jnp.float32)
        partial_value = partial_value + jnp.dot(conv_mixed[:, conv_lo:conv_lo + conv_part], convolution_output_matrix[:, conv_lo:conv_lo + conv_part].T, preferred_element_type=jnp.float32)
        total = total + lax.optimization_barrier(partial_value.astype(jnp.bfloat16)).astype(jnp.float32)
    return total.astype(jnp.bfloat16)
```

```python
import jax
import jax.numpy as jnp
from jax import lax
from jax.experimental import pallas as pl
from jax.experimental.pallas import tpu as pltpu
from jax.sharding import Mesh
from jax.sharding import PartitionSpec as P

BF = jnp.bfloat16
F32 = jnp.float32
NN = (((1,), (0,)), ((), ()))
NT = (((1,), (1,)), ((), ()))
TN = (((0,), (0,)), ((), ()))

SP = ("za", "zb", "zc", "y")
Z = ("za", "zb", "zc")
TP = ("x", "c")
FAR = ("za", "zb")
NEAR = ("zc", "y")
RMS_EPSILON = 1e-06
GROUP_EPSILON = 0.00064
LAYER_EPSILON = 1e-05
UNIT_EPSILON = 1e-06

TOK = 256
HALO = 32
RB = 32
DIM = 2048
STATS = 16


def dot1(a, b, dims=NN):
    return lax.dot_general(a.astype(BF), b.astype(BF), dims, preferred_element_type=F32)


def two(a):
    hi = a.astype(BF)
    return hi, (a - hi.astype(F32)).astype(BF)


def dot3(a, b, dims=NN):
    ah, al = two(a)
    bh, bl = two(b)
    one = lambda l, r: lax.dot_general(l, r, dims, preferred_element_type=F32)
    return one(ah, bh) + (one(ah, bl) + one(al, bh))


def three(a):
    hi = a.astype(BF)
    rest = a - hi.astype(F32)
    mid = rest.astype(BF)
    return hi, mid, (rest - mid.astype(F32)).astype(BF)


def lanes(shape):
    return lax.broadcasted_iota(jnp.int32, shape, len(shape) - 1)


def rows(shape):
    return lax.broadcasted_iota(jnp.int32, shape, 0)


def by_head(pair, shape):
    return jnp.where(lanes(shape) < 64, pair[:, 0:1], pair[:, 1:2])


def head_sum(a):
    first = lanes(a.shape) < 64
    s0 = jnp.sum(jnp.where(first, a, 0.0), axis=1, keepdims=True)
    s1 = jnp.sum(jnp.where(first, 0.0, a), axis=1, keepdims=True)
    return jnp.where(first, s0, s1)


def rms_rows(x, gain):
    x = x.astype(F32)
    scale = lax.rsqrt(jnp.mean(x * x, axis=-1, keepdims=True) + RMS_EPSILON)
    return (x * scale * gain).astype(BF)


def norm_kernel(tok, gain, df, ds, do, lf, ls, lo, fr, sr, normed, rates):
    x = rms_rows(tok[...], gain[...])
    normed[...] = x
    mid = jnp.tanh(dot1(x, df[...])).astype(BF)
    pre = do[...] + dot1(mid, ds[...])
    rate = 0.6065306597126334 / (1.0 + jnp.exp(-pre))
    step = by_head(jnp.log(sr[...]), rate.shape) - rate * by_head(fr[...], rate.shape)
    rates[0] = step
    low = (rows((TOK, TOK)) >= lanes((TOK, TOK))).astype(BF)
    h, m, l = three(step)
    rates[1] = dot1(low, h) + (dot1(low, m) + dot1(low, l))
    mid2 = dot1(x, lf[...]).astype(BF)
    pre2 = lo[...] + dot1(mid2, ls[...])
    rates[2] = 1.0 / (1.0 + jnp.exp(-pre2))


def in_row_order(w, ws):
    for y in range(4):
        for z in range(16):
            ws[z, y] = w[y, z]


def state_kernel(x, w, rates, parts, trans, ws, ew, ek, qw, qk):
    in_row_order(w, ws)
    proj = dot1(x[...], ws[...].reshape(DIM, 384))
    q, k, v = proj[:, :128], proj[:, 128:256], proj[:, 256:]
    g = rates[1]
    before = g - rates[0]
    unit = k * lax.rsqrt(head_sum(k * k) + UNIT_EPSILON)
    er = -unit
    wr = unit * rates[2]
    first32 = lanes((RB, 128)) < 64
    for i in range(TOK // RB):
        lo, hi = i * RB, (i + 1) * RB
        width = 128 if hi <= 128 else 256
        ref = g[lo + RB // 2 - 1 : lo + RB // 2]
        le = er[lo:hi] * jnp.exp(before[lo:hi] - ref)
        lq = q[lo:hi] * jnp.exp(g[lo:hi] - ref)
        left = jnp.concatenate(
            [
                jnp.where(first32, le, 0.0),
                jnp.where(first32, 0.0, le),
                jnp.where(first32, lq, 0.0),
                jnp.where(first32, 0.0, lq),
            ],
            axis=0,
        ).astype(BF)
        dec = jnp.exp(jnp.minimum(ref - g[:width], 60.0))
        pw = dot1(left, wr[:width] * dec, NT)
        pk = dot1(left, k[:width] * dec, NT)
        t = rows((RB, width)) + lo
        s = lanes((RB, width))
        strict, incl = t > s, t >= s
        for h in range(2):
            a, b = h * RB, (h + 1) * RB
            c, d = (2 + h) * RB, (3 + h) * RB
            ew[h, lo:hi, :width] = jnp.where(strict, pw[a:b], 0.0).astype(BF)
            ek[h, lo:hi, :width] = jnp.where(strict, pk[a:b], 0.0)
            qw[h, lo:hi, :width] = jnp.where(incl, pw[c:d], 0.0)
            qk[h, lo:hi, :width] = jnp.where(incl, pk[c:d], 0.0)
            if width < TOK:
                zero = jnp.zeros((RB, TOK - width), F32)
                ew[h, lo:hi, width:] = zero.astype(BF)
                ek[h, lo:hi, width:] = zero
                qw[h, lo:hi, width:] = zero
                qk[h, lo:hi, width:] = zero
    t = rows((TOK, TOK))
    s = lanes((TOK, TOK))

    def same(n):
        return (t // n) == (s // n)

    invs = []
    base = [jnp.where(same(8), ew[h], jnp.zeros((), BF)) for h in range(2)]
    sq = [dot1(n8, n8) for n8 in base]
    eye = (t == s).astype(F32)
    cube = [dot1(n8, n2) for n8, n2 in zip(base, sq)]
    four = [dot1(n2, n2) for n2 in sq]
    part = [eye + n8.astype(F32) + n2 + n3 for n8, n2, n3 in zip(base, sq, cube)]
    invs = [p + dot1(p, n4) for p, n4 in zip(part, four)]
    for n in (8, 16, 32, 64):
        off = same(2 * n) & ~same(n)
        xs = [
            dot1(jnp.where(off, ew[h], jnp.zeros((), BF)), invs[h])
            for h in range(2)
        ]
        invs = [inv + dot1(inv, xx) for inv, xx in zip(invs, xs)]
    first = lanes((TOK, 128)) < 64
    ehat = er * jnp.exp(before)
    qhat = q * jnp.exp(g)
    last = g[TOK - 1 : TOK]
    toend = jnp.exp(last - g)
    wend = wr * toend
    kend = k * toend
    vsw = pltpu.roll(v, 64, axis=1)
    ys, zs = [], []
    for h in range(2):
        own = first if h == 0 else ~first
        r = jnp.where(own, ehat, dot3(ek[h], vsw))
        inv = invs[h]
        x1 = dot3(inv[:128, :128], r[:128])
        r2 = r[128:] + dot3(ew[h, 128:, :128].astype(F32), x1)
        x2 = dot3(inv[128:, 128:], r2)
        xx = jnp.concatenate([x1, x2], axis=0)
        ys.append(dot3(qw[h], xx) + jnp.where(own, qhat, dot3(qk[h], vsw)))
        zz = dot3(xx, wend, TN)
        zs.append(zz if h == 0 else jnp.concatenate([zz[64:], zz[:64]], axis=0))
    parts[0] = jnp.where(first, ys[0], ys[1])
    parts[1] = pltpu.roll(jnp.where(first, ys[1], ys[0]), 64, axis=1)
    vk = dot3(v, kend, TN)
    half = lanes((64, 128)) < 64
    diag = (lanes((64, 128)) % 64) == rows((64, 128))
    dpart = jnp.where(half, zs[0][:64], zs[1][:64]) + jnp.where(diag, jnp.exp(last) - 1.0, 0.0)
    ppart = jnp.where(half, zs[0][64:] + vk[:64], zs[1][64:] + vk[64:])
    trans[...] = jnp.concatenate([dpart, ppart], axis=0).astype(BF)


def two_blocks(a):
    half = lanes((64, 128)) < 64
    return jnp.concatenate([jnp.where(half, a, 0.0), jnp.where(half, 0.0, a)], axis=0)


def chain(earlier, later):
    d, p = earlier
    turn = two_blocks(later[0])
    d, p = d + later[0] + dot3(d, turn), p + later[1] + dot3(p, turn)
    return jnp.minimum(d, 3e38), jnp.minimum(p, 3e38)


def fold(pieces):
    while len(pieces) > 1:
        pieces = [chain(pieces[k], pieces[k + 1]) for k in range(0, len(pieces), 2)]
    return pieces[0]


def unpacked(ref):
    return [(ref[k, :64].astype(F32), ref[k, 64:].astype(F32)) for k in range(8)]


def passed(place, pieces):
    keep = [place[0] > k for k in range(8)]
    return [(jnp.where(on, d, 0.0), jnp.where(on, p, 0.0)) for on, (d, p) in zip(keep, pieces)]


def prefix_kernel(place, pieces, total, prefix):
    each = unpacked(pieces)
    d, p = fold(each)
    total[:64] = d.astype(BF)
    total[64:] = p.astype(BF)
    d, p = fold(passed(place, each))
    prefix[:64] = d
    prefix[64:] = p


def finish_kernel(place, pieces, before, parts, gain, dev, pay):
    inside = fold(passed(place, unpacked(pieces)))
    state = chain(inside, (before[:64], before[64:]))[1]
    y = parts[1] + dot3(parts[0], two_blocks(state), NT)
    c = y - head_sum(y) * (1.0 / 64.0)
    n = c * lax.rsqrt(head_sum(c * c) * (1.0 / 64.0) + GROUP_EPSILON)
    mixed = (n * gain[...]).astype(BF)
    pay[: TOK + STATS] = dev[...]
    pay[TOK + STATS :, :128] = mixed[:128]
    pay[TOK + STATS :, 128:] = mixed[128:]


def from_neighbours(place, pieces, ws):
    for k, piece in enumerate(pieces):
        y = lax.rem(place[0] + 4 - k, 4)
        for z in range(16):
            ws[z, y] = piece[z]


def conv_kernel(place, x, halo, gain, w0, w1, w2, w3, taps, cgain, out, ws, gs):
    from_neighbours(place, (w0, w1, w2, w3), ws)
    wide = ws[...].reshape(DIM, 512)
    ph = dot1(rms_rows(halo[...], gain[...]), wide)
    pm = dot1(x[...], wide)

    def gate(p):
        return (p[:, :256] / (1.0 + jnp.exp(-p[:, 256:]))).astype(BF).astype(F32)

    gs[:HALO] = gate(ph)
    gs[HALO:] = gate(pm)
    acc = jnp.zeros((TOK, 256), F32)
    for j in range(31):
        acc = acc + taps[j : j + 1] * gs[pl.ds(2 + j, TOK), :]
    mean = jnp.mean(acc, axis=1, keepdims=True)
    dev = acc - mean
    sq = jnp.sum(dev * dev, axis=1, keepdims=True)
    out[:TOK] = dev.astype(BF)
    parts = [p.astype(F32) for p in (*three(mean), *three(sq))]
    col = lanes((TOK, 128))
    grid = jnp.zeros((TOK, 128), F32)
    for k, p in enumerate(parts):
        grid = jnp.where(col == k, p, grid)
    low = jnp.transpose(grid)[:STATS]
    r = rows((STATS, 256))
    for k, p in enumerate(three(cgain[...])):
        low = jnp.where(r == 6 + k, p.astype(F32), low)
    out[TOK:] = low.astype(BF)


def final_kernel(place, pay, w0, w1, w2, w3, out, shifts):
    low = pay[:, TOK : TOK + STATS].astype(F32).reshape(8 * STATS, 256)
    cols = jnp.transpose(low)

    def stat(g, k):
        c = g * STATS + k
        return cols[:, c : c + 1] + cols[:, c + 1 : c + 2] + cols[:, c + 2 : c + 3]

    means = [stat(g, 0) for g in range(8)]
    mean = sum(means) * 0.125
    var = sum(stat(g, 3) for g in range(8))
    var = (var + 256.0 * sum((m - mean) * (m - mean) for m in means)) * (1.0 / 2048.0)
    inv = lax.rsqrt(var + LAYER_EPSILON)
    for g in range(8):
        shifts[g] = jnp.broadcast_to((means[g] - mean) * inv, (TOK, 128))
    total = jnp.zeros((TOK, 256), F32)
    for k, piece in enumerate((w0, w1, w2, w3)):
        y = lax.rem(place[0] + 4 - k, 4)
        for half in range(2):
            g = 2 * y + half
            w = piece[8 * half : 8 * half + 8].reshape(256, 384)
            head = pay[g, TOK : TOK + STATS].astype(F32)
            gain = head[6:7] + head[7:8] + head[8:9]
            shift = shifts[g]
            u = pay[g, :TOK].astype(F32) * inv + jnp.concatenate([shift, shift], axis=1)
            u = u * gain
            u = u / (1.0 + jnp.exp(-u))
            total = total + dot1(u, w[:, 128:], NT)
            m = pay[g, TOK + STATS :]
            m = jnp.concatenate([m[:, :128], m[:, 128:]], axis=0)
            total = total + dot1(m, w[:, :128], NT)
    out[...] = total.astype(BF)


def place_kernel(place, own, other, out, sems):
    c = place[0]
    copies = []
    for x in range(4):
        for k, (src, core) in enumerate(((own, c), (other, 1 - c))):
            at = pl.multiple_of((2 * x + core) * 256, 256)
            copies.append(
                pltpu.make_async_copy(src.at[x], out.at[:, pl.ds(at, 256)], sems.at[2 * x + k])
            )
    for copy in copies:
        copy.start()
    for copy in copies:
        copy.wait()


VM = pl.BlockSpec(memory_space=pltpu.VMEM)
SM = pl.BlockSpec(memory_space=pltpu.SMEM)


def call(kernel, outs, args, scratch=(), smem=0):
    return pl.pallas_call(
        kernel,
        out_shape=[jax.ShapeDtypeStruct(s, d) for s, d in outs],
        in_specs=[SM] * smem + [VM] * (len(args) - smem),
        out_specs=[VM] * len(outs),
        scratch_shapes=list(scratch),
        compiler_params=pltpu.CompilerParams(vmem_limit_bytes=24 * 1024 * 1024),
    )(*args)


def everyone(x, axis):
    size = lax.axis_size(axis)
    copies = jnp.broadcast_to(x, (size, *x.shape))
    return lax.all_to_all(copies, axis, split_axis=0, concat_axis=0, tiled=True)


def placed(axis):
    return lax.axis_index(axis).reshape(1).astype(jnp.int32)


def neighbours(x):
    pieces = [x]
    for k in (1, 2, 3):
        pieces.append(lax.ppermute(x, "y", [(i, (i + k) % 4) for i in range(4)]))
    return pieces


def layer(
    tokens,
    input_norm_gain,
    query_matrix,
    key_matrix,
    value_matrix,
    convolution_value_matrix,
    convolution_gate_matrix,
    decay_offset_channel,
    decay_first_matrix,
    decay_second_matrix,
    learning_rate_offset,
    learning_rate_first_matrix,
    learning_rate_second_matrix,
    forgetting_rate_factor,
    state_retention_share,
    per_head_norm_gain,
    convolution_filter_taps,
    convolution_channel_gain,
    attention_output_matrix,
    convolution_output_matrix,
):
    row = lambda a: a.reshape(1, -1)
    gain = row(input_norm_gain)
    w_state = jnp.concatenate([query_matrix, key_matrix, value_matrix], axis=1)
    w_out = jnp.concatenate([attention_output_matrix, convolution_output_matrix], axis=1)
    w_state = everyone(everyone(w_state, Z), "y")
    halo = lax.ppermute(tokens[TOK - HALO :], SP, [(i, i + 1) for i in range(63)])
    moves = []
    for a in range(8):
        for b in range(8):
            for j in range(8):
                target = ((j % 2) * 8 + b) * 4 + j // 2
                moves.append(((8 * a + b) * 8 + j, target * 8 + a))
    w_out = lax.ppermute(w_out, (*SP, *TP), moves)
    rest = jnp.concatenate([convolution_value_matrix, convolution_gate_matrix, w_out], axis=1)
    rest = lax.all_gather(rest, Z)
    w_conv = neighbours(rest[..., :512])
    w_out = neighbours(rest[..., 512:])

    normed, rates = call(
        norm_kernel,
        [((TOK, DIM), BF), ((3, TOK, 128), F32)],
        (
            tokens,
            gain,
            decay_first_matrix,
            decay_second_matrix,
            row(decay_offset_channel),
            learning_rate_first_matrix,
            learning_rate_second_matrix,
            row(learning_rate_offset),
            forgetting_rate_factor,
            state_retention_share,
        ),
    )
    square = pltpu.VMEM((2, TOK, TOK), F32)
    parts, trans = call(
        state_kernel,
        [((2, TOK, 128), F32), ((128, 128), BF)],
        (normed, w_state, rates),
        [pltpu.VMEM((16, 4, 32, 384), BF), pltpu.VMEM((2, TOK, TOK), BF), square, square, square],
    )

    total, before = call(
        prefix_kernel,
        [((128, 128), BF), ((128, 128), F32)],
        (placed(NEAR), everyone(trans, NEAR)),
        smem=1,
    )
    y = placed("y")
    (dev,) = call(
        conv_kernel,
        [((TOK + STATS, 256), BF)],
        (y, normed, halo, gain, *w_conv, convolution_filter_taps, row(convolution_channel_gain)),
        [pltpu.VMEM((16, 4, 32, 512), BF), pltpu.VMEM((TOK + HALO, 256), F32)],
        smem=1,
    )
    (pay,) = call(
        finish_kernel,
        [((TOK + STATS + 128, 256), BF)],
        (placed(FAR), everyone(total, FAR), before, parts, row(per_head_norm_gain), dev),
        smem=1,
    )
    (out,) = call(
        final_kernel,
        [((TOK, 256), BF)],
        (y, everyone(pay, TP), *w_out),
        [pltpu.VMEM((8, TOK, 128), F32)],
        smem=1,
    )
    own = everyone(out, "x")
    other = lax.ppermute(own, "c", [(0, 1), (1, 0)])
    hbm = pl.BlockSpec(memory_space=pl.ANY)
    return pl.pallas_call(
        place_kernel,
        out_shape=jax.ShapeDtypeStruct((TOK, DIM), BF),
        in_specs=[SM, VM, VM],
        out_specs=hbm,
        scratch_shapes=[pltpu.SemaphoreType.DMA((8,))],
        name="place",
    )(placed("c"), own, other)


def solution(mesh):
    finer = Mesh(mesh.devices.reshape(4, 2, 2, 4, 4, 2), (*SP, *TP))
    return jax.shard_map(
        layer,
        mesh=finer,
        in_specs=(
            P(SP, None),
            P(),
            P(SP, TP),
            P(SP, TP),
            P(SP, TP),
            P(SP, TP),
            P(SP, TP),
            P(TP),
            P(),
            P(None, TP),
            P(TP),
            P(),
            P(None, TP),
            P(SP, TP),
            P(SP, TP),
            P(TP),
            P(None, TP),
            P(TP),
            P(SP, TP),
            P(SP, TP),
        ),
        out_specs=P(SP, None),
        check_vma=False,
    )
```

```python
import jax
import jax.numpy as jnp
from jax import lax
from jax.experimental import pallas as pl
from jax.experimental.pallas import tpu as pltpu
from jax.sharding import Mesh
from jax.sharding import PartitionSpec as P

BF = jnp.bfloat16
F32 = jnp.float32
NN = (((1,), (0,)), ((), ()))
NT = (((1,), (1,)), ((), ()))
TN = (((0,), (0,)), ((), ()))

SP = ("za", "zb", "zc", "y")
Z = ("za", "zb", "zc")
TP = ("x", "c")
FAR = ("za", "zb")
NEAR = ("zc", "y")
RMS_EPSILON = 1e-06
GROUP_EPSILON = 0.00064
LAYER_EPSILON = 1e-05
UNIT_EPSILON = 1e-06

TOK = 256
HALO = 32
RB = 32
DIM = 2048
STATS = 16


def dot1(a, b, dims=NN):
    return lax.dot_general(a.astype(BF), b.astype(BF), dims, preferred_element_type=F32)


def two(a):
    hi = a.astype(BF)
    return hi, (a - hi.astype(F32)).astype(BF)


def dot3(a, b, dims=NN):
    ah, al = two(a)
    bh, bl = two(b)
    one = lambda l, r: lax.dot_general(l, r, dims, preferred_element_type=F32)
    return one(ah, bh) + (one(ah, bl) + one(al, bh))


def three(a):
    hi = a.astype(BF)
    rest = a - hi.astype(F32)
    mid = rest.astype(BF)
    return hi, mid, (rest - mid.astype(F32)).astype(BF)


def lanes(shape):
    return lax.broadcasted_iota(jnp.int32, shape, len(shape) - 1)


def rows(shape):
    return lax.broadcasted_iota(jnp.int32, shape, 0)


def by_head(pair, shape):
    return jnp.where(lanes(shape) < 64, pair[:, 0:1], pair[:, 1:2])


def head_sum(a):
    first = lanes(a.shape) < 64
    s0 = jnp.sum(jnp.where(first, a, 0.0), axis=1, keepdims=True)
    s1 = jnp.sum(jnp.where(first, 0.0, a), axis=1, keepdims=True)
    return jnp.where(first, s0, s1)


def rms_rows(x, gain):
    x = x.astype(F32)
    scale = lax.rsqrt(jnp.mean(x * x, axis=-1, keepdims=True) + RMS_EPSILON)
    return (x * scale * gain).astype(BF)


def norm_kernel(tok, gain, df, ds, do, lf, ls, lo, fr, sr, normed, rates):
    x = rms_rows(tok[...], gain[...])
    normed[...] = x
    mid = jnp.tanh(dot1(x, df[...])).astype(BF)
    pre = do[...] + dot1(mid, ds[...])
    rate = 0.6065306597126334 / (1.0 + jnp.exp(-pre))
    step = by_head(jnp.log(sr[...]), rate.shape) - rate * by_head(fr[...], rate.shape)
    rates[0] = step
    low = (rows((TOK, TOK)) >= lanes((TOK, TOK))).astype(BF)
    h, m, l = three(step)
    rates[1] = dot1(low, h) + (dot1(low, m) + dot1(low, l))
    mid2 = dot1(x, lf[...]).astype(BF)
    pre2 = lo[...] + dot1(mid2, ls[...])
    rates[2] = 1.0 / (1.0 + jnp.exp(-pre2))


def in_row_order(w, ws):
    for y in range(4):
        for z in range(16):
            ws[z, y] = w[y, z]


def state_kernel(x, w, rates, parts, trans, ws, ew, ek, qw, qk):
    in_row_order(w, ws)
    proj = dot1(x[...], ws[...].reshape(DIM, 384))
    q, k, v = proj[:, :128], proj[:, 128:256], proj[:, 256:]
    g = rates[1]
    before = g - rates[0]
    unit = k * lax.rsqrt(head_sum(k * k) + UNIT_EPSILON)
    er = -unit
    wr = unit * rates[2]
    first32 = lanes((RB, 128)) < 64
    for i in range(TOK // RB):
        lo, hi = i * RB, (i + 1) * RB
        width = 128 if hi <= 128 else 256
        ref = g[lo + RB // 2 - 1 : lo + RB // 2]
        le = er[lo:hi] * jnp.exp(before[lo:hi] - ref)
        lq = q[lo:hi] * jnp.exp(g[lo:hi] - ref)
        left = jnp.concatenate(
            [
                jnp.where(first32, le, 0.0),
                jnp.where(first32, 0.0, le),
                jnp.where(first32, lq, 0.0),
                jnp.where(first32, 0.0, lq),
            ],
            axis=0,
        ).astype(BF)
        dec = jnp.exp(jnp.minimum(ref - g[:width], 60.0))
        pw = dot1(left, wr[:width] * dec, NT)
        pk = dot1(left, k[:width] * dec, NT)
        t = rows((RB, width)) + lo
        s = lanes((RB, width))
        strict, incl = t > s, t >= s
        for h in range(2):
            a, b = h * RB, (h + 1) * RB
            c, d = (2 + h) * RB, (3 + h) * RB
            ew[h, lo:hi, :width] = jnp.where(strict, pw[a:b], 0.0).astype(BF)
            ek[h, lo:hi, :width] = jnp.where(strict, pk[a:b], 0.0)
            qw[h, lo:hi, :width] = jnp.where(incl, pw[c:d], 0.0)
            qk[h, lo:hi, :width] = jnp.where(incl, pk[c:d], 0.0)
            if width < TOK:
                zero = jnp.zeros((RB, TOK - width), F32)
                ew[h, lo:hi, width:] = zero.astype(BF)
                ek[h, lo:hi, width:] = zero
                qw[h, lo:hi, width:] = zero
                qk[h, lo:hi, width:] = zero
    t = rows((TOK, TOK))
    s = lanes((TOK, TOK))

    def same(n):
        return (t // n) == (s // n)

    invs = []
    base = [jnp.where(same(8), ew[h], jnp.zeros((), BF)) for h in range(2)]
    sq = [dot1(n8, n8) for n8 in base]
    eye = (t == s).astype(F32)
    cube = [dot1(n8, n2) for n8, n2 in zip(base, sq)]
    four = [dot1(n2, n2) for n2 in sq]
    part = [eye + n8.astype(F32) + n2 + n3 for n8, n2, n3 in zip(base, sq, cube)]
    invs = [p + dot1(p, n4) for p, n4 in zip(part, four)]
    for n in (8, 16, 32, 64):
        off = same(2 * n) & ~same(n)
        xs = [
            dot1(jnp.where(off, ew[h], jnp.zeros((), BF)), invs[h])
            for h in range(2)
        ]
        invs = [inv + dot1(inv, xx) for inv, xx in zip(invs, xs)]
    first = lanes((TOK, 128)) < 64
    ehat = er * jnp.exp(before)
    qhat = q * jnp.exp(g)
    last = g[TOK - 1 : TOK]
    toend = jnp.exp(last - g)
    wend = wr * toend
    kend = k * toend
    vsw = pltpu.roll(v, 64, axis=1)
    ys, zs = [], []
    for h in range(2):
        own = first if h == 0 else ~first
        r = jnp.where(own, ehat, dot3(ek[h], vsw))
        inv = invs[h]
        x1 = dot3(inv[:128, :128], r[:128])
        r2 = r[128:] + dot3(ew[h, 128:, :128].astype(F32), x1)
        x2 = dot3(inv[128:, 128:], r2)
        xx = jnp.concatenate([x1, x2], axis=0)
        ys.append(dot3(qw[h], xx) + jnp.where(own, qhat, dot3(qk[h], vsw)))
        zz = dot3(xx, wend, TN)
        zs.append(zz if h == 0 else jnp.concatenate([zz[64:], zz[:64]], axis=0))
    parts[0] = jnp.where(first, ys[0], ys[1])
    parts[1] = pltpu.roll(jnp.where(first, ys[1], ys[0]), 64, axis=1)
    vk = dot3(v, kend, TN)
    half = lanes((64, 128)) < 64
    diag = (lanes((64, 128)) % 64) == rows((64, 128))
    dpart = jnp.where(half, zs[0][:64], zs[1][:64]) + jnp.where(diag, jnp.exp(last) - 1.0, 0.0)
    ppart = jnp.where(half, zs[0][64:] + vk[:64], zs[1][64:] + vk[64:])
    mine = jnp.concatenate([dpart, ppart], axis=0).astype(BF)
    for k in range(8):
        trans[k] = mine


def two_blocks(a):
    half = lanes((64, 128)) < 64
    return jnp.concatenate([jnp.where(half, a, 0.0), jnp.where(half, 0.0, a)], axis=0)


def chain(earlier, later):
    d, p = earlier
    turn = two_blocks(later[0])
    d, p = d + later[0] + dot3(d, turn), p + later[1] + dot3(p, turn)
    return jnp.minimum(d, 3e38), jnp.minimum(p, 3e38)


def fold(pieces):
    while len(pieces) > 1:
        pieces = [chain(pieces[k], pieces[k + 1]) for k in range(0, len(pieces), 2)]
    return pieces[0]


def unpacked(ref):
    return [(ref[k, :64].astype(F32), ref[k, 64:].astype(F32)) for k in range(8)]


def passed(place, pieces):
    keep = [place[0] > k for k in range(8)]
    return [(jnp.where(on, d, 0.0), jnp.where(on, p, 0.0)) for on, (d, p) in zip(keep, pieces)]


def prefix_kernel(place, pieces, total, prefix):
    each = unpacked(pieces)
    d, p = fold(each)
    d, p = d.astype(BF), p.astype(BF)
    for k in range(8):
        total[k, :64] = d
        total[k, 64:] = p
    d, p = fold(passed(place, each))
    prefix[:64] = d
    prefix[64:] = p


def finish_kernel(place, pieces, before, parts, gain, dev, pay):
    inside = fold(passed(place, unpacked(pieces)))
    state = chain(inside, (before[:64], before[64:]))[1]
    y = parts[1] + dot3(parts[0], two_blocks(state), NT)
    c = y - head_sum(y) * (1.0 / 64.0)
    n = c * lax.rsqrt(head_sum(c * c) * (1.0 / 64.0) + GROUP_EPSILON)
    mixed = (n * gain[...]).astype(BF)
    rows_ = dev[...]
    for k in range(4):
        pay[k, : TOK + STATS] = rows_
        pay[k, TOK + STATS :, :128] = mixed[:128]
        pay[k, TOK + STATS :, 128:] = mixed[128:]


def from_neighbours(place, pieces, ws):
    for k, piece in enumerate(pieces):
        y = lax.rem(place[0] + 4 - k, 4)
        for z in range(16):
            ws[z, y] = piece[z]


def conv_kernel(place, x, halo, gain, w0, w1, w2, w3, taps, cgain, out, ws, gs):
    from_neighbours(place, (w0, w1, w2, w3), ws)
    wide = ws[...].reshape(DIM, 512)
    ph = dot1(rms_rows(halo[...], gain[...]), wide)
    pm = dot1(x[...], wide)

    def gate(p):
        return (p[:, :256] / (1.0 + jnp.exp(-p[:, 256:]))).astype(BF).astype(F32)

    gs[:HALO] = gate(ph)
    gs[HALO:] = gate(pm)
    acc = jnp.zeros((TOK, 256), F32)
    for j in range(31):
        acc = acc + taps[j : j + 1] * gs[pl.ds(2 + j, TOK), :]
    mean = jnp.mean(acc, axis=1, keepdims=True)
    dev = acc - mean
    sq = jnp.sum(dev * dev, axis=1, keepdims=True)
    out[:TOK] = dev.astype(BF)
    parts = [p.astype(F32) for p in (*three(mean), *three(sq))]
    col = lanes((TOK, 128))
    grid = jnp.zeros((TOK, 128), F32)
    for k, p in enumerate(parts):
        grid = jnp.where(col == k, p, grid)
    low = jnp.transpose(grid)[:STATS]
    r = rows((STATS, 256))
    for k, p in enumerate(three(cgain[...])):
        low = jnp.where(r == 6 + k, p.astype(F32), low)
    out[TOK:] = low.astype(BF)


def final_kernel(place, core, own, other, w0, w1, w2, w3, out, shifts):
    low = jnp.concatenate(
        [p[:, TOK : TOK + STATS].astype(F32).reshape(4 * STATS, 256) for p in (own, other)], axis=0
    )
    cols = jnp.transpose(low)

    def stat(g, k):
        c = g * STATS + k
        return cols[:, c : c + 1] + cols[:, c + 1 : c + 2] + cols[:, c + 2 : c + 3]

    means = [stat(g, 0) for g in range(8)]
    mean = sum(means) * 0.125
    var = sum(stat(g, 3) for g in range(8))
    var = (var + 256.0 * sum((m - mean) * (m - mean) for m in means)) * (1.0 / 2048.0)
    inv = lax.rsqrt(var + LAYER_EPSILON)
    for g in range(8):
        shifts[g] = jnp.broadcast_to((means[g] - mean) * inv, (TOK, 128))
    total = jnp.zeros((TOK, 256), F32)
    for k, piece in enumerate((w0, w1, w2, w3)):
        x = lax.rem(place[0] + 4 - k, 4)
        for n, pay in enumerate((own, other)):
            half = core[0] if n == 0 else 1 - core[0]
            w = piece[pl.ds(half * 8, 8)].reshape(256, 384)
            head = pay[x, TOK : TOK + STATS].astype(F32)
            gain = head[6:7] + head[7:8] + head[8:9]
            shift = shifts[4 * n + x]
            u = pay[x, :TOK].astype(F32) * inv + jnp.concatenate([shift, shift], axis=1)
            u = u * gain
            u = u / (1.0 + jnp.exp(-u))
            total = total + dot1(u, w[:, 128:], NT)
            m = pay[x, TOK + STATS :]
            m = jnp.concatenate([m[:, :128], m[:, 128:]], axis=0)
            total = total + dot1(m, w[:, :128], NT)
    total = total.astype(BF)
    for k in range(4):
        out[k] = total


def place_kernel(place, own, other, out, sems):
    c = place[0]
    copies = []
    for x in range(4):
        for k, (src, core) in enumerate(((own, c), (other, 1 - c))):
            at = pl.multiple_of((2 * x + core) * 256, 256)
            copies.append(
                pltpu.make_async_copy(src.at[x], out.at[:, pl.ds(at, 256)], sems.at[2 * x + k])
            )
    for copy in copies:
        copy.start()
    for copy in copies:
        copy.wait()


VM = pl.BlockSpec(memory_space=pltpu.VMEM)
SM = pl.BlockSpec(memory_space=pltpu.SMEM)


def call(kernel, outs, args, scratch=(), smem=0):
    return pl.pallas_call(
        kernel,
        out_shape=[jax.ShapeDtypeStruct(s, d) for s, d in outs],
        in_specs=[SM] * smem + [VM] * (len(args) - smem),
        out_specs=[VM] * len(outs),
        scratch_shapes=list(scratch),
        compiler_params=pltpu.CompilerParams(vmem_limit_bytes=24 * 1024 * 1024),
    )(*args)


def everyone(x, axis):
    size = lax.axis_size(axis)
    copies = jnp.broadcast_to(x, (size, *x.shape))
    return lax.all_to_all(copies, axis, split_axis=0, concat_axis=0, tiled=True)


def exchange(copies, axis):
    return lax.all_to_all(copies, axis, split_axis=0, concat_axis=0, tiled=True)


def other_core(x):
    return lax.ppermute(x, "c", [(0, 1), (1, 0)])


def placed(axis):
    return lax.axis_index(axis).reshape(1).astype(jnp.int32)


def neighbours(x):
    pieces = [x]
    for k in (1, 2, 3):
        pieces.append(lax.ppermute(x, "y", [(i, (i + k) % 4) for i in range(4)]))
    return pieces


def layer(
    tokens,
    input_norm_gain,
    query_matrix,
    key_matrix,
    value_matrix,
    convolution_value_matrix,
    convolution_gate_matrix,
    decay_offset_channel,
    decay_first_matrix,
    decay_second_matrix,
    learning_rate_offset,
    learning_rate_first_matrix,
    learning_rate_second_matrix,
    forgetting_rate_factor,
    state_retention_share,
    per_head_norm_gain,
    convolution_filter_taps,
    convolution_channel_gain,
    attention_output_matrix,
    convolution_output_matrix,
):
    row = lambda a: a.reshape(1, -1)
    gain = row(input_norm_gain)
    w_state = jnp.concatenate([query_matrix, key_matrix, value_matrix], axis=1)
    w_out = jnp.concatenate([attention_output_matrix, convolution_output_matrix], axis=1)
    w_state = everyone(everyone(w_state, Z), "y")
    halo = lax.ppermute(tokens[TOK - HALO :], SP, [(i, i + 1) for i in range(63)])
    moves = []
    for a in range(8):
        for b in range(8):
            for j in range(8):
                target = ((j % 2) * 8 + b) * 4 + j // 2
                moves.append(((8 * a + b) * 8 + j, target * 8 + a))
    w_out = lax.ppermute(w_out, (*SP, *TP), moves)
    rest = jnp.concatenate([convolution_value_matrix, convolution_gate_matrix, w_out], axis=1)
    rest = lax.all_gather(rest, Z)
    w_conv = neighbours(rest[..., :512])
    w_out = neighbours(rest[..., 512:])

    normed, rates = call(
        norm_kernel,
        [((TOK, DIM), BF), ((3, TOK, 128), F32)],
        (
            tokens,
            gain,
            decay_first_matrix,
            decay_second_matrix,
            row(decay_offset_channel),
            learning_rate_first_matrix,
            learning_rate_second_matrix,
            row(learning_rate_offset),
            forgetting_rate_factor,
            state_retention_share,
        ),
    )
    square = pltpu.VMEM((2, TOK, TOK), F32)
    parts, trans = call(
        state_kernel,
        [((2, TOK, 128), F32), ((8, 128, 128), BF)],
        (normed, w_state, rates),
        [pltpu.VMEM((16, 4, 32, 384), BF), pltpu.VMEM((2, TOK, TOK), BF), square, square, square],
    )

    total, before = call(
        prefix_kernel,
        [((8, 128, 128), BF), ((128, 128), F32)],
        (placed(NEAR), exchange(trans, NEAR)),
        smem=1,
    )
    y = placed("y")
    (dev,) = call(
        conv_kernel,
        [((TOK + STATS, 256), BF)],
        (y, normed, halo, gain, *w_conv, convolution_filter_taps, row(convolution_channel_gain)),
        [pltpu.VMEM((16, 4, 32, 512), BF), pltpu.VMEM((TOK + HALO, 256), F32)],
        smem=1,
    )
    (pay,) = call(
        finish_kernel,
        [((4, TOK + STATS + 128, 256), BF)],
        (placed(FAR), exchange(total, FAR), before, parts, row(per_head_norm_gain), dev),
        smem=1,
    )
    pay = exchange(pay, "x")
    (out,) = call(
        final_kernel,
        [((4, TOK, 256), BF)],
        (y, placed("c"), pay, other_core(pay), *w_out),
        [pltpu.VMEM((8, TOK, 128), F32)],
        smem=2,
    )
    own = exchange(out, "x")
    other = other_core(own)
    hbm = pl.BlockSpec(memory_space=pl.ANY)
    return pl.pallas_call(
        place_kernel,
        out_shape=jax.ShapeDtypeStruct((TOK, DIM), BF),
        in_specs=[SM, VM, VM],
        out_specs=hbm,
        scratch_shapes=[pltpu.SemaphoreType.DMA((8,))],
        name="place",
    )(placed("c"), own, other)


def solution(mesh):
    finer = Mesh(mesh.devices.reshape(4, 2, 2, 4, 4, 2), (*SP, *TP))
    return jax.shard_map(
        layer,
        mesh=finer,
        in_specs=(
            P(SP, None),
            P(),
            P(SP, TP),
            P(SP, TP),
            P(SP, TP),
            P(SP, TP),
            P(SP, TP),
            P(TP),
            P(),
            P(None, TP),
            P(TP),
            P(),
            P(None, TP),
            P(SP, TP),
            P(SP, TP),
            P(TP),
            P(None, TP),
            P(TP),
            P(SP, TP),
            P(SP, TP),
        ),
        out_specs=P(SP, None),
        check_vma=False,
    )
```

```python
import jax
import jax.numpy as jnp
from jax import lax
from jax.experimental import pallas as pl
from jax.experimental.pallas import tpu as pltpu
from jax.sharding import Mesh
from jax.sharding import PartitionSpec as P

BF = jnp.bfloat16
F32 = jnp.float32
NN = (((1,), (0,)), ((), ()))
NT = (((1,), (1,)), ((), ()))
TN = (((0,), (0,)), ((), ()))

SP = ("za", "zb", "zc", "y")
Z = ("za", "zb", "zc")
TP = ("x", "c")
FAR = "za"
NEAR = ("zb", "zc", "y")
RMS_EPSILON = 1e-06
GROUP_EPSILON = 0.00064
LAYER_EPSILON = 1e-05
UNIT_EPSILON = 1e-06

TOK = 256
HALO = 32
RB = 32
DIM = 2048
STATS = 16


def dot1(a, b, dims=NN):
    return lax.dot_general(a.astype(BF), b.astype(BF), dims, preferred_element_type=F32)


def two(a):
    hi = a.astype(BF)
    return hi, (a - hi.astype(F32)).astype(BF)


def dot3(a, b, dims=NN):
    ah, al = two(a)
    bh, bl = two(b)
    one = lambda l, r: lax.dot_general(l, r, dims, preferred_element_type=F32)
    return one(ah, bh) + (one(ah, bl) + one(al, bh))


def three(a):
    hi = a.astype(BF)
    rest = a - hi.astype(F32)
    mid = rest.astype(BF)
    return hi, mid, (rest - mid.astype(F32)).astype(BF)


def lanes(shape):
    return lax.broadcasted_iota(jnp.int32, shape, len(shape) - 1)


def rows(shape):
    return lax.broadcasted_iota(jnp.int32, shape, 0)


def by_head(pair, shape):
    return jnp.where(lanes(shape) < 64, pair[:, 0:1], pair[:, 1:2])


def head_sum(a):
    first = lanes(a.shape) < 64
    s0 = jnp.sum(jnp.where(first, a, 0.0), axis=1, keepdims=True)
    s1 = jnp.sum(jnp.where(first, 0.0, a), axis=1, keepdims=True)
    return jnp.where(first, s0, s1)


def rms_rows(x, gain):
    x = x.astype(F32)
    scale = lax.rsqrt(jnp.mean(x * x, axis=-1, keepdims=True) + RMS_EPSILON)
    return (x * scale * gain).astype(BF)


def norm_kernel(tok, gain, df, ds, do, lf, ls, lo, fr, sr, normed, rates):
    x = rms_rows(tok[...], gain[...])
    normed[...] = x
    mid = jnp.tanh(dot1(x, df[...])).astype(BF)
    pre = do[...] + dot1(mid, ds[...])
    rate = 0.6065306597126334 / (1.0 + jnp.exp(-pre))
    step = by_head(jnp.log(sr[...]), rate.shape) - rate * by_head(fr[...], rate.shape)
    rates[0] = step
    low = (rows((TOK, TOK)) >= lanes((TOK, TOK))).astype(BF)
    h, m, l = three(step)
    rates[1] = dot1(low, h) + (dot1(low, m) + dot1(low, l))
    mid2 = dot1(x, lf[...]).astype(BF)
    pre2 = lo[...] + dot1(mid2, ls[...])
    rates[2] = 1.0 / (1.0 + jnp.exp(-pre2))


def in_row_order(w, ws):
    for y in range(4):
        for z in range(16):
            ws[z, y] = w[y, z]


def state_kernel(x, w, rates, parts, trans, ws, ew, ek, qw, qk):
    in_row_order(w, ws)
    proj = dot1(x[...], ws[...].reshape(DIM, 384))
    q, k, v = proj[:, :128], proj[:, 128:256], proj[:, 256:]
    g = rates[1]
    before = g - rates[0]
    unit = k * lax.rsqrt(head_sum(k * k) + UNIT_EPSILON)
    er = -unit
    wr = unit * rates[2]
    first32 = lanes((RB, 128)) < 64
    for i in range(TOK // RB):
        lo, hi = i * RB, (i + 1) * RB
        width = 128 if hi <= 128 else 256
        ref = g[lo + RB // 2 - 1 : lo + RB // 2]
        le = er[lo:hi] * jnp.exp(before[lo:hi] - ref)
        lq = q[lo:hi] * jnp.exp(g[lo:hi] - ref)
        left = jnp.concatenate(
            [
                jnp.where(first32, le, 0.0),
                jnp.where(first32, 0.0, le),
                jnp.where(first32, lq, 0.0),
                jnp.where(first32, 0.0, lq),
            ],
            axis=0,
        ).astype(BF)
        dec = jnp.exp(jnp.minimum(ref - g[:width], 60.0))
        pw = dot1(left, wr[:width] * dec, NT)
        pk = dot1(left, k[:width] * dec, NT)
        t = rows((RB, width)) + lo
        s = lanes((RB, width))
        strict, incl = t > s, t >= s
        for h in range(2):
            a, b = h * RB, (h + 1) * RB
            c, d = (2 + h) * RB, (3 + h) * RB
            ew[h, lo:hi, :width] = jnp.where(strict, pw[a:b], 0.0).astype(BF)
            ek[h, lo:hi, :width] = jnp.where(strict, pk[a:b], 0.0)
            qw[h, lo:hi, :width] = jnp.where(incl, pw[c:d], 0.0)
            qk[h, lo:hi, :width] = jnp.where(incl, pk[c:d], 0.0)
            if width < TOK:
                zero = jnp.zeros((RB, TOK - width), F32)
                ew[h, lo:hi, width:] = zero.astype(BF)
                ek[h, lo:hi, width:] = zero
                qw[h, lo:hi, width:] = zero
                qk[h, lo:hi, width:] = zero
    t = rows((TOK, TOK))
    s = lanes((TOK, TOK))

    def same(n):
        return (t // n) == (s // n)

    invs = []
    base = [jnp.where(same(8), ew[h], jnp.zeros((), BF)) for h in range(2)]
    sq = [dot1(n8, n8) for n8 in base]
    eye = (t == s).astype(F32)
    cube = [dot1(n8, n2) for n8, n2 in zip(base, sq)]
    four = [dot1(n2, n2) for n2 in sq]
    part = [eye + n8.astype(F32) + n2 + n3 for n8, n2, n3 in zip(base, sq, cube)]
    invs = [p + dot1(p, n4) for p, n4 in zip(part, four)]
    for n in (8, 16, 32, 64):
        off = same(2 * n) & ~same(n)
        xs = [
            dot1(jnp.where(off, ew[h], jnp.zeros((), BF)), invs[h])
            for h in range(2)
        ]
        invs = [inv + dot1(inv, xx) for inv, xx in zip(invs, xs)]
    first = lanes((TOK, 128)) < 64
    ehat = er * jnp.exp(before)
    qhat = q * jnp.exp(g)
    last = g[TOK - 1 : TOK]
    toend = jnp.exp(last - g)
    wend = wr * toend
    kend = k * toend
    vsw = pltpu.roll(v, 64, axis=1)
    ys, zs = [], []
    for h in range(2):
        own = first if h == 0 else ~first
        r = jnp.where(own, ehat, dot3(ek[h], vsw))
        inv = invs[h]
        x1 = dot3(inv[:128, :128], r[:128])
        r2 = r[128:] + dot3(ew[h, 128:, :128].astype(F32), x1)
        x2 = dot3(inv[128:, 128:], r2)
        xx = jnp.concatenate([x1, x2], axis=0)
        ys.append(dot3(qw[h], xx) + jnp.where(own, qhat, dot3(qk[h], vsw)))
        zz = dot3(xx, wend, TN)
        zs.append(zz if h == 0 else jnp.concatenate([zz[64:], zz[:64]], axis=0))
    parts[0] = jnp.where(first, ys[0], ys[1])
    parts[1] = pltpu.roll(jnp.where(first, ys[1], ys[0]), 64, axis=1)
    vk = dot3(v, kend, TN)
    half = lanes((64, 128)) < 64
    diag = (lanes((64, 128)) % 64) == rows((64, 128))
    dpart = jnp.where(half, zs[0][:64], zs[1][:64]) + jnp.where(diag, jnp.exp(last) - 1.0, 0.0)
    ppart = jnp.where(half, zs[0][64:] + vk[:64], zs[1][64:] + vk[64:])
    mine = jnp.concatenate([dpart, ppart], axis=0).astype(BF)
    for k in range(16):
        trans[k] = mine


def two_blocks(a):
    half = lanes((64, 128)) < 64
    return jnp.concatenate([jnp.where(half, a, 0.0), jnp.where(half, 0.0, a)], axis=0)


def chain(earlier, later):
    d, p = earlier
    turn = two_blocks(later[0])
    d, p = d + later[0] + dot3(d, turn), p + later[1] + dot3(p, turn)
    return jnp.minimum(d, 3e38), jnp.minimum(p, 3e38)


def fold(pieces):
    while len(pieces) > 1:
        pieces = [chain(pieces[k], pieces[k + 1]) for k in range(0, len(pieces), 2)]
    return pieces[0]


def unpacked(ref):
    return [(ref[k, :64].astype(F32), ref[k, 64:].astype(F32)) for k in range(ref.shape[0])]


def passed(place, pieces):
    keep = [place[0] > k for k in range(len(pieces))]
    return [(jnp.where(on, d, 0.0), jnp.where(on, p, 0.0)) for on, (d, p) in zip(keep, pieces)]


def prefix_kernel(place, pieces, total, prefix):
    each = unpacked(pieces)
    d, p = fold(each)
    d, p = d.astype(BF), p.astype(BF)
    for k in range(4):
        total[k, :64] = d
        total[k, 64:] = p
    d, p = fold(passed(place, each))
    prefix[:64] = d
    prefix[64:] = p


def finish_kernel(place, pieces, before, parts, gain, dev, pay):
    inside = fold(passed(place, unpacked(pieces)))
    state = chain(inside, (before[:64], before[64:]))[1]
    y = parts[1] + dot3(parts[0], two_blocks(state), NT)
    c = y - head_sum(y) * (1.0 / 64.0)
    n = c * lax.rsqrt(head_sum(c * c) * (1.0 / 64.0) + GROUP_EPSILON)
    mixed = (n * gain[...]).astype(BF)
    rows_ = dev[...]
    for k in range(4):
        pay[k, : TOK + STATS] = rows_
        pay[k, TOK + STATS :, :128] = mixed[:128]
        pay[k, TOK + STATS :, 128:] = mixed[128:]


def from_neighbours(place, pieces, ws):
    for k, piece in enumerate(pieces):
        y = lax.rem(place[0] + 4 - k, 4)
        for z in range(16):
            ws[z, y] = piece[z]


def conv_kernel(place, x, halo, gain, w0, w1, w2, w3, taps, cgain, out, ws, gs):
    from_neighbours(place, (w0, w1, w2, w3), ws)
    wide = ws[...].reshape(DIM, 512)
    ph = dot1(rms_rows(halo[...], gain[...]), wide)
    pm = dot1(x[...], wide)

    def gate(p):
        return (p[:, :256] / (1.0 + jnp.exp(-p[:, 256:]))).astype(BF).astype(F32)

    gs[:HALO] = gate(ph)
    gs[HALO:] = gate(pm)
    acc = jnp.zeros((TOK, 256), F32)
    for j in range(31):
        acc = acc + taps[j : j + 1] * gs[pl.ds(2 + j, TOK), :]
    mean = jnp.mean(acc, axis=1, keepdims=True)
    dev = acc - mean
    sq = jnp.sum(dev * dev, axis=1, keepdims=True)
    out[:TOK] = dev.astype(BF)
    parts = [p.astype(F32) for p in (*three(mean), *three(sq))]
    col = lanes((TOK, 128))
    grid = jnp.zeros((TOK, 128), F32)
    for k, p in enumerate(parts):
        grid = jnp.where(col == k, p, grid)
    low = jnp.transpose(grid)[:STATS]
    r = rows((STATS, 256))
    for k, p in enumerate(three(cgain[...])):
        low = jnp.where(r == 6 + k, p.astype(F32), low)
    out[TOK:] = low.astype(BF)


def final_kernel(place, core, own, other, w0, w1, w2, w3, out, shifts):
    low = jnp.concatenate(
        [p[:, TOK : TOK + STATS].astype(F32).reshape(4 * STATS, 256) for p in (own, other)], axis=0
    )
    cols = jnp.transpose(low)

    def stat(g, k):
        c = g * STATS + k
        return cols[:, c : c + 1] + cols[:, c + 1 : c + 2] + cols[:, c + 2 : c + 3]

    means = [stat(g, 0) for g in range(8)]
    mean = sum(means) * 0.125
    var = sum(stat(g, 3) for g in range(8))
    var = (var + 256.0 * sum((m - mean) * (m - mean) for m in means)) * (1.0 / 2048.0)
    inv = lax.rsqrt(var + LAYER_EPSILON)
    for g in range(8):
        shifts[g] = jnp.broadcast_to((means[g] - mean) * inv, (TOK, 128))
    total = jnp.zeros((TOK, 256), F32)
    for k, piece in enumerate((w0, w1, w2, w3)):
        x = lax.rem(place[0] + 4 - k, 4)
        for n, pay in enumerate((own, other)):
            half = core[0] if n == 0 else 1 - core[0]
            w = piece[pl.ds(half * 8, 8)].reshape(256, 384)
            head = pay[x, TOK : TOK + STATS].astype(F32)
            gain = head[6:7] + head[7:8] + head[8:9]
            shift = shifts[4 * n + x]
            u = pay[x, :TOK].astype(F32) * inv + jnp.concatenate([shift, shift], axis=1)
            u = u * gain
            u = u / (1.0 + jnp.exp(-u))
            total = total + dot1(u, w[:, 128:], NT)
            m = pay[x, TOK + STATS :]
            m = jnp.concatenate([m[:, :128], m[:, 128:]], axis=0)
            total = total + dot1(m, w[:, :128], NT)
    total = total.astype(BF)
    for k in range(4):
        out[k] = total


def place_kernel(place, own, other, out, sems):
    c = place[0]
    copies = []
    for x in range(4):
        for k, (src, core) in enumerate(((own, c), (other, 1 - c))):
            at = pl.multiple_of((2 * x + core) * 256, 256)
            copies.append(
                pltpu.make_async_copy(src.at[x], out.at[:, pl.ds(at, 256)], sems.at[2 * x + k])
            )
    for copy in copies:
        copy.start()
    for copy in copies:
        copy.wait()


VM = pl.BlockSpec(memory_space=pltpu.VMEM)
SM = pl.BlockSpec(memory_space=pltpu.SMEM)


def call(kernel, outs, args, scratch=(), smem=0):
    return pl.pallas_call(
        kernel,
        out_shape=[jax.ShapeDtypeStruct(s, d) for s, d in outs],
        in_specs=[SM] * smem + [VM] * (len(args) - smem),
        out_specs=[VM] * len(outs),
        scratch_shapes=list(scratch),
        compiler_params=pltpu.CompilerParams(vmem_limit_bytes=24 * 1024 * 1024),
    )(*args)


def everyone(x, axis):
    size = lax.axis_size(axis)
    copies = jnp.broadcast_to(x, (size, *x.shape))
    return lax.all_to_all(copies, axis, split_axis=0, concat_axis=0, tiled=True)


def exchange(copies, axis):
    return lax.all_to_all(copies, axis, split_axis=0, concat_axis=0, tiled=True)


def other_core(x):
    return lax.ppermute(x, "c", [(0, 1), (1, 0)])


def placed(axis):
    return lax.axis_index(axis).reshape(1).astype(jnp.int32)


def neighbours(x):
    pieces = [x]
    for k in (1, 2, 3):
        pieces.append(lax.ppermute(x, "y", [(i, (i + k) % 4) for i in range(4)]))
    return pieces


def layer(
    tokens,
    input_norm_gain,
    query_matrix,
    key_matrix,
    value_matrix,
    convolution_value_matrix,
    convolution_gate_matrix,
    decay_offset_channel,
    decay_first_matrix,
    decay_second_matrix,
    learning_rate_offset,
    learning_rate_first_matrix,
    learning_rate_second_matrix,
    forgetting_rate_factor,
    state_retention_share,
    per_head_norm_gain,
    convolution_filter_taps,
    convolution_channel_gain,
    attention_output_matrix,
    convolution_output_matrix,
):
    row = lambda a: a.reshape(1, -1)
    gain = row(input_norm_gain)
    w_state = jnp.concatenate([query_matrix, key_matrix, value_matrix], axis=1)
    w_out = jnp.concatenate([attention_output_matrix, convolution_output_matrix], axis=1)
    w_state = everyone(everyone(w_state, Z), "y")
    halo = lax.ppermute(tokens[TOK - HALO :], SP, [(i, i + 1) for i in range(63)])
    moves = []
    for a in range(8):
        for b in range(8):
            for j in range(8):
                target = ((j % 2) * 8 + b) * 4 + j // 2
                moves.append(((8 * a + b) * 8 + j, target * 8 + a))
    w_out = lax.ppermute(w_out, (*SP, *TP), moves)
    rest = jnp.concatenate([convolution_value_matrix, convolution_gate_matrix, w_out], axis=1)
    rest = lax.all_gather(rest, Z)
    w_conv = neighbours(rest[..., :512])
    w_out = neighbours(rest[..., 512:])

    normed, rates = call(
        norm_kernel,
        [((TOK, DIM), BF), ((3, TOK, 128), F32)],
        (
            tokens,
            gain,
            decay_first_matrix,
            decay_second_matrix,
            row(decay_offset_channel),
            learning_rate_first_matrix,
            learning_rate_second_matrix,
            row(learning_rate_offset),
            forgetting_rate_factor,
            state_retention_share,
        ),
    )
    square = pltpu.VMEM((2, TOK, TOK), F32)
    parts, trans = call(
        state_kernel,
        [((2, TOK, 128), F32), ((16, 128, 128), BF)],
        (normed, w_state, rates),
        [pltpu.VMEM((16, 4, 32, 384), BF), pltpu.VMEM((2, TOK, TOK), BF), square, square, square],
    )

    total, before = call(
        prefix_kernel,
        [((4, 128, 128), BF), ((128, 128), F32)],
        (placed(NEAR), exchange(trans, NEAR)),
        smem=1,
    )
    y = placed("y")
    (dev,) = call(
        conv_kernel,
        [((TOK + STATS, 256), BF)],
        (y, normed, halo, gain, *w_conv, convolution_filter_taps, row(convolution_channel_gain)),
        [pltpu.VMEM((16, 4, 32, 512), BF), pltpu.VMEM((TOK + HALO, 256), F32)],
        smem=1,
    )
    (pay,) = call(
        finish_kernel,
        [((4, TOK + STATS + 128, 256), BF)],
        (placed(FAR), exchange(total, FAR), before, parts, row(per_head_norm_gain), dev),
        smem=1,
    )
    pay = exchange(pay, "x")
    (out,) = call(
        final_kernel,
        [((4, TOK, 256), BF)],
        (y, placed("c"), pay, other_core(pay), *w_out),
        [pltpu.VMEM((8, TOK, 128), F32)],
        smem=2,
    )
    own = exchange(out, "x")
    other = other_core(own)
    hbm = pl.BlockSpec(memory_space=pl.ANY)
    return pl.pallas_call(
        place_kernel,
        out_shape=jax.ShapeDtypeStruct((TOK, DIM), BF),
        in_specs=[SM, VM, VM],
        out_specs=hbm,
        scratch_shapes=[pltpu.SemaphoreType.DMA((8,))],
        name="place",
    )(placed("c"), own, other)


def solution(mesh):
    finer = Mesh(mesh.devices.reshape(4, 2, 2, 4, 4, 2), (*SP, *TP))
    return jax.shard_map(
        layer,
        mesh=finer,
        in_specs=(
            P(SP, None),
            P(),
            P(SP, TP),
            P(SP, TP),
            P(SP, TP),
            P(SP, TP),
            P(SP, TP),
            P(TP),
            P(),
            P(None, TP),
            P(TP),
            P(),
            P(None, TP),
            P(SP, TP),
            P(SP, TP),
            P(TP),
            P(None, TP),
            P(TP),
            P(SP, TP),
            P(SP, TP),
        ),
        out_specs=P(SP, None),
        check_vma=False,
    )
```

```python
import jax
import jax.numpy as jnp
from jax import lax
from jax.experimental import pallas as pl
from jax.experimental.pallas import tpu as pltpu
from jax.sharding import Mesh
from jax.sharding import PartitionSpec as P

BF = jnp.bfloat16
F32 = jnp.float32
NN = (((1,), (0,)), ((), ()))
NT = (((1,), (1,)), ((), ()))
TN = (((0,), (0,)), ((), ()))

SP = ("za", "zb", "zc", "y")
Z = ("za", "zb", "zc")
TP = ("x", "c")
FAR = "za"
NEAR = ("zb", "zc", "y")
RMS_EPSILON = 1e-06
GROUP_EPSILON = 0.00064
LAYER_EPSILON = 1e-05
UNIT_EPSILON = 1e-06

TOK = 256
HALO = 32
RB = 32
DIM = 2048
STATS = 16


def dot1(a, b, dims=NN):
    return lax.dot_general(a.astype(BF), b.astype(BF), dims, preferred_element_type=F32)


def two(a):
    hi = a.astype(BF)
    return hi, (a - hi.astype(F32)).astype(BF)


def dot3(a, b, dims=NN):
    ah, al = two(a)
    bh, bl = two(b)
    one = lambda l, r: lax.dot_general(l, r, dims, preferred_element_type=F32)
    return one(ah, bh) + (one(ah, bl) + one(al, bh))


def three(a):
    hi = a.astype(BF)
    rest = a - hi.astype(F32)
    mid = rest.astype(BF)
    return hi, mid, (rest - mid.astype(F32)).astype(BF)


def lanes(shape):
    return lax.broadcasted_iota(jnp.int32, shape, len(shape) - 1)


def rows(shape):
    return lax.broadcasted_iota(jnp.int32, shape, 0)


def by_head(pair, shape):
    return jnp.where(lanes(shape) < 64, pair[:, 0:1], pair[:, 1:2])


def head_sum(a):
    first = lanes(a.shape) < 64
    s0 = jnp.sum(jnp.where(first, a, 0.0), axis=1, keepdims=True)
    s1 = jnp.sum(jnp.where(first, 0.0, a), axis=1, keepdims=True)
    return jnp.where(first, s0, s1)


def rms_rows(x, gain):
    x = x.astype(F32)
    scale = lax.rsqrt(jnp.mean(x * x, axis=-1, keepdims=True) + RMS_EPSILON)
    return (x * scale * gain).astype(BF)


def norm_kernel(tok, gain, df, ds, do, lf, ls, lo, fr, sr, normed, rates):
    x = rms_rows(tok[...], gain[...])
    normed[...] = x
    mid = jnp.tanh(dot1(x, df[...])).astype(BF)
    pre = do[...] + dot1(mid, ds[...])
    rate = 0.6065306597126334 / (1.0 + jnp.exp(-pre))
    step = by_head(jnp.log(sr[...]), rate.shape) - rate * by_head(fr[...], rate.shape)
    rates[0] = step
    low = (rows((TOK, TOK)) >= lanes((TOK, TOK))).astype(BF)
    h, m, l = three(step)
    rates[1] = dot1(low, h) + (dot1(low, m) + dot1(low, l))
    mid2 = dot1(x, lf[...]).astype(BF)
    pre2 = lo[...] + dot1(mid2, ls[...])
    rates[2] = 1.0 / (1.0 + jnp.exp(-pre2))


def in_row_order(w, ws):
    for y in range(4):
        for z in range(16):
            ws[z, y] = w[y, z]


def state_kernel(x, w, rates, parts, trans, ws, ew, ek, qw, qk):
    in_row_order(w, ws)
    proj = dot1(x[...], ws[...].reshape(DIM, 384))
    q, k, v = proj[:, :128], proj[:, 128:256], proj[:, 256:]
    g = rates[1]
    before = g - rates[0]
    unit = k * lax.rsqrt(head_sum(k * k) + UNIT_EPSILON)
    er = -unit
    wr = unit * rates[2]
    first32 = lanes((RB, 128)) < 64
    for i in range(TOK // RB):
        lo, hi = i * RB, (i + 1) * RB
        width = 128 if hi <= 128 else 256
        ref = g[lo + RB // 2 - 1 : lo + RB // 2]
        le = er[lo:hi] * jnp.exp(before[lo:hi] - ref)
        lq = q[lo:hi] * jnp.exp(g[lo:hi] - ref)
        left = jnp.concatenate(
            [
                jnp.where(first32, le, 0.0),
                jnp.where(first32, 0.0, le),
                jnp.where(first32, lq, 0.0),
                jnp.where(first32, 0.0, lq),
            ],
            axis=0,
        ).astype(BF)
        dec = jnp.exp(jnp.minimum(ref - g[:width], 60.0))
        pw = dot1(left, wr[:width] * dec, NT)
        pk = dot1(left, k[:width] * dec, NT)
        t = rows((RB, width)) + lo
        s = lanes((RB, width))
        strict, incl = t > s, t >= s
        for h in range(2):
            a, b = h * RB, (h + 1) * RB
            c, d = (2 + h) * RB, (3 + h) * RB
            ew[h, lo:hi, :width] = jnp.where(strict, pw[a:b], 0.0).astype(BF)
            ek[h, lo:hi, :width] = jnp.where(strict, pk[a:b], 0.0)
            qw[h, lo:hi, :width] = jnp.where(incl, pw[c:d], 0.0)
            qk[h, lo:hi, :width] = jnp.where(incl, pk[c:d], 0.0)
            if width < TOK:
                zero = jnp.zeros((RB, TOK - width), F32)
                ew[h, lo:hi, width:] = zero.astype(BF)
                ek[h, lo:hi, width:] = zero
                qw[h, lo:hi, width:] = zero
                qk[h, lo:hi, width:] = zero
    t = rows((TOK, TOK))
    s = lanes((TOK, TOK))

    def same(n):
        return (t // n) == (s // n)

    invs = []
    base = [jnp.where(same(8), ew[h], jnp.zeros((), BF)) for h in range(2)]
    sq = [dot1(n8, n8) for n8 in base]
    eye = (t == s).astype(F32)
    cube = [dot1(n8, n2) for n8, n2 in zip(base, sq)]
    four = [dot1(n2, n2) for n2 in sq]
    part = [eye + n8.astype(F32) + n2 + n3 for n8, n2, n3 in zip(base, sq, cube)]
    invs = [p + dot1(p, n4) for p, n4 in zip(part, four)]
    for n in (8, 16, 32, 64):
        off = same(2 * n) & ~same(n)
        xs = [
            dot1(jnp.where(off, ew[h], jnp.zeros((), BF)), invs[h])
            for h in range(2)
        ]
        invs = [inv + dot1(inv, xx) for inv, xx in zip(invs, xs)]
    first = lanes((TOK, 128)) < 64
    ehat = er * jnp.exp(before)
    qhat = q * jnp.exp(g)
    last = g[TOK - 1 : TOK]
    toend = jnp.exp(last - g)
    wend = wr * toend
    kend = k * toend
    vsw = pltpu.roll(v, 64, axis=1)
    ys, zs = [], []
    for h in range(2):
        own = first if h == 0 else ~first
        r = jnp.where(own, ehat, dot3(ek[h], vsw))
        inv = invs[h]
        x1 = dot3(inv[:128, :128], r[:128])
        r2 = r[128:] + dot3(ew[h, 128:, :128].astype(F32), x1)
        x2 = dot3(inv[128:, 128:], r2)
        xx = jnp.concatenate([x1, x2], axis=0)
        ys.append(dot3(qw[h], xx) + jnp.where(own, qhat, dot3(qk[h], vsw)))
        zz = dot3(xx, wend, TN)
        zs.append(zz if h == 0 else jnp.concatenate([zz[64:], zz[:64]], axis=0))
    parts[0] = jnp.where(first, ys[0], ys[1])
    parts[1] = pltpu.roll(jnp.where(first, ys[1], ys[0]), 64, axis=1)
    vk = dot3(v, kend, TN)
    half = lanes((64, 128)) < 64
    diag = (lanes((64, 128)) % 64) == rows((64, 128))
    dpart = jnp.where(half, zs[0][:64], zs[1][:64]) + jnp.where(diag, jnp.exp(last) - 1.0, 0.0)
    ppart = jnp.where(half, zs[0][64:] + vk[:64], zs[1][64:] + vk[64:])
    mine = jnp.concatenate([dpart, ppart], axis=0).astype(BF)
    for k in range(16):
        trans[k] = mine


def two_blocks(a):
    half = lanes((64, 128)) < 64
    return jnp.concatenate([jnp.where(half, a, 0.0), jnp.where(half, 0.0, a)], axis=0)


def chain(earlier, later):
    d, p = earlier
    turn = two_blocks(later[0])
    d, p = d + later[0] + dot3(d, turn), p + later[1] + dot3(p, turn)
    return jnp.minimum(d, 3e38), jnp.minimum(p, 3e38)


def fold(pieces):
    while len(pieces) > 1:
        pieces = [chain(pieces[k], pieces[k + 1]) for k in range(0, len(pieces), 2)]
    return pieces[0]


def unpacked(ref):
    return [(ref[k, :64].astype(F32), ref[k, 64:].astype(F32)) for k in range(ref.shape[0])]


def passed(place, pieces):
    keep = [place[0] > k for k in range(len(pieces))]
    return [(jnp.where(on, d, 0.0), jnp.where(on, p, 0.0)) for on, (d, p) in zip(keep, pieces)]


def prefix_kernel(place, pieces, total, prefix):
    each = unpacked(pieces)
    d, p = fold(each)
    d, p = d.astype(BF), p.astype(BF)
    for k in range(4):
        total[k, :64] = d
        total[k, 64:] = p
    d, p = fold(passed(place, each))
    prefix[:64] = d
    prefix[64:] = p


def finish_kernel(place, pieces, before, parts, gain, dev, pay):
    inside = fold(passed(place, unpacked(pieces)))
    state = chain(inside, (before[:64], before[64:]))[1]
    y = parts[1] + dot3(parts[0], two_blocks(state), NT)
    c = y - head_sum(y) * (1.0 / 64.0)
    n = c * lax.rsqrt(head_sum(c * c) * (1.0 / 64.0) + GROUP_EPSILON)
    mixed = (n * gain[...]).astype(BF)
    rows_ = dev[...]
    for k in range(4):
        pay[k, : TOK + STATS] = rows_
        pay[k, TOK + STATS :, :128] = mixed[:128]
        pay[k, TOK + STATS :, 128:] = mixed[128:]


def from_neighbours(place, pieces, ws):
    for k, piece in enumerate(pieces):
        y = lax.rem(place[0] + 4 - k, 4)
        for z in range(16):
            ws[z, y] = piece[z]


def conv_kernel(place, x, halo, gain, w0, w1, w2, w3, taps, cgain, out, ws, gs):
    from_neighbours(place, (w0, w1, w2, w3), ws)
    wide = ws[...].reshape(DIM, 512)
    ph = dot1(rms_rows(halo[...], gain[...]), wide)
    pm = dot1(x[...], wide)

    def gate(p):
        return (p[:, :256] / (1.0 + jnp.exp(-p[:, 256:]))).astype(BF).astype(F32)

    gs[:HALO] = gate(ph)
    gs[HALO:] = gate(pm)
    acc = jnp.zeros((TOK, 256), F32)
    for j in range(31):
        acc = acc + taps[j : j + 1] * gs[pl.ds(2 + j, TOK), :]
    mean = jnp.mean(acc, axis=1, keepdims=True)
    dev = acc - mean
    sq = jnp.sum(dev * dev, axis=1, keepdims=True)
    out[:TOK] = dev.astype(BF)
    parts = [p.astype(F32) for p in (*three(mean), *three(sq))]
    col = lanes((TOK, 128))
    grid = jnp.zeros((TOK, 128), F32)
    for k, p in enumerate(parts):
        grid = jnp.where(col == k, p, grid)
    low = jnp.transpose(grid)[:STATS]
    r = rows((STATS, 256))
    for k, p in enumerate(three(cgain[...])):
        low = jnp.where(r == 6 + k, p.astype(F32), low)
    out[TOK:] = low.astype(BF)


def final_kernel(place, core, own, other, w0, w1, w2, w3, out, shifts):
    low = jnp.concatenate(
        [p[:, TOK : TOK + STATS].astype(F32).reshape(4 * STATS, 256) for p in (own, other)], axis=0
    )
    cols = jnp.transpose(low)

    def stat(g, k):
        c = g * STATS + k
        return cols[:, c : c + 1] + cols[:, c + 1 : c + 2] + cols[:, c + 2 : c + 3]

    means = [stat(g, 0) for g in range(8)]
    mean = sum(means) * 0.125
    var = sum(stat(g, 3) for g in range(8))
    var = (var + 256.0 * sum((m - mean) * (m - mean) for m in means)) * (1.0 / 2048.0)
    inv = lax.rsqrt(var + LAYER_EPSILON)
    for g in range(8):
        shifts[g] = jnp.broadcast_to((means[g] - mean) * inv, (TOK, 128))
    total = jnp.zeros((TOK, 256), F32)
    for k, piece in enumerate((w0, w1, w2, w3)):
        x = lax.rem(place[0] + 4 - k, 4)
        for n, pay in enumerate((own, other)):
            half = core[0] if n == 0 else 1 - core[0]
            w = piece[pl.ds(half * 8, 8)].reshape(256, 384)
            head = pay[x, TOK : TOK + STATS].astype(F32)
            gain = head[6:7] + head[7:8] + head[8:9]
            shift = shifts[4 * n + x]
            u = pay[x, :TOK].astype(F32) * inv + jnp.concatenate([shift, shift], axis=1)
            u = u * gain
            u = u / (1.0 + jnp.exp(-u))
            total = total + dot1(u, w[:, 128:], NT)
            m = pay[x, TOK + STATS :]
            m = jnp.concatenate([m[:, :128], m[:, 128:]], axis=0)
            total = total + dot1(m, w[:, :128], NT)
    total = total.astype(BF)
    for k in range(4):
        out[k] = total


def fan_kernel(x, out):
    for k in range(4):
        out[k] = x[...]


def place_blocks(core, blocks, out, sems):
    copies = []
    for x in range(4):
        at = pl.multiple_of((2 * x + core) * 256, 256)
        copies.append(pltpu.make_async_copy(blocks.at[x], out.at[:, pl.ds(at, 256)], sems.at[x]))
    for copy in copies:
        copy.start()
    for copy in copies:
        copy.wait()


def place_own(place, own, out, sems):
    place_blocks(place[0], own, out, sems)


def place_other(place, other, begun, out, sems):
    place_blocks(1 - place[0], other, out, sems)


VM = pl.BlockSpec(memory_space=pltpu.VMEM)
SM = pl.BlockSpec(memory_space=pltpu.SMEM)


def call(kernel, outs, args, scratch=(), smem=0):
    return pl.pallas_call(
        kernel,
        out_shape=[jax.ShapeDtypeStruct(s, d) for s, d in outs],
        in_specs=[SM] * smem + [VM] * (len(args) - smem),
        out_specs=[VM] * len(outs),
        scratch_shapes=list(scratch),
        compiler_params=pltpu.CompilerParams(vmem_limit_bytes=24 * 1024 * 1024),
    )(*args)


def everyone(x, axis):
    size = lax.axis_size(axis)
    copies = jnp.broadcast_to(x, (size, *x.shape))
    return lax.all_to_all(copies, axis, split_axis=0, concat_axis=0, tiled=True)


def exchange(copies, axis):
    return lax.all_to_all(copies, axis, split_axis=0, concat_axis=0, tiled=True)


def other_core(x):
    return lax.ppermute(x, "c", [(0, 1), (1, 0)])


def placed(axis):
    return lax.axis_index(axis).reshape(1).astype(jnp.int32)


def neighbours(x):
    pieces = [x]
    for k in (1, 2, 3):
        pieces.append(lax.ppermute(x, "y", [(i, (i + k) % 4) for i in range(4)]))
    return pieces


def layer(
    tokens,
    input_norm_gain,
    query_matrix,
    key_matrix,
    value_matrix,
    convolution_value_matrix,
    convolution_gate_matrix,
    decay_offset_channel,
    decay_first_matrix,
    decay_second_matrix,
    learning_rate_offset,
    learning_rate_first_matrix,
    learning_rate_second_matrix,
    forgetting_rate_factor,
    state_retention_share,
    per_head_norm_gain,
    convolution_filter_taps,
    convolution_channel_gain,
    attention_output_matrix,
    convolution_output_matrix,
):
    row = lambda a: a.reshape(1, -1)
    gain = row(input_norm_gain)
    w_state = jnp.concatenate([query_matrix, key_matrix, value_matrix], axis=1)
    w_out = jnp.concatenate([attention_output_matrix, convolution_output_matrix], axis=1)
    w_state = everyone(w_state, Z)
    (w_state,) = call(fan_kernel, [((4, 16, 32, 384), BF)], (w_state,))
    w_state = exchange(w_state, "y")
    halo = lax.ppermute(tokens[TOK - HALO :], SP, [(i, i + 1) for i in range(63)])
    moves = []
    for a in range(8):
        for b in range(8):
            for j in range(8):
                target = ((j % 2) * 8 + b) * 4 + j // 2
                moves.append(((8 * a + b) * 8 + j, target * 8 + a))
    w_out = lax.ppermute(w_out, (*SP, *TP), moves)
    rest = jnp.concatenate([convolution_value_matrix, convolution_gate_matrix, w_out], axis=1)
    rest = lax.all_gather(rest, Z)
    w_conv = neighbours(rest[..., :512])
    w_out = neighbours(rest[..., 512:])

    normed, rates = call(
        norm_kernel,
        [((TOK, DIM), BF), ((3, TOK, 128), F32)],
        (
            tokens,
            gain,
            decay_first_matrix,
            decay_second_matrix,
            row(decay_offset_channel),
            learning_rate_first_matrix,
            learning_rate_second_matrix,
            row(learning_rate_offset),
            forgetting_rate_factor,
            state_retention_share,
        ),
    )
    square = pltpu.VMEM((2, TOK, TOK), F32)
    parts, trans = call(
        state_kernel,
        [((2, TOK, 128), F32), ((16, 128, 128), BF)],
        (normed, w_state, rates),
        [pltpu.VMEM((16, 4, 32, 384), BF), pltpu.VMEM((2, TOK, TOK), BF), square, square, square],
    )

    total, before = call(
        prefix_kernel,
        [((4, 128, 128), BF), ((128, 128), F32)],
        (placed(NEAR), exchange(trans, NEAR)),
        smem=1,
    )
    y = placed("y")
    (dev,) = call(
        conv_kernel,
        [((TOK + STATS, 256), BF)],
        (y, normed, halo, gain, *w_conv, convolution_filter_taps, row(convolution_channel_gain)),
        [pltpu.VMEM((16, 4, 32, 512), BF), pltpu.VMEM((TOK + HALO, 256), F32)],
        smem=1,
    )
    (pay,) = call(
        finish_kernel,
        [((4, TOK + STATS + 128, 256), BF)],
        (placed(FAR), exchange(total, FAR), before, parts, row(per_head_norm_gain), dev),
        smem=1,
    )
    pay = exchange(pay, "x")
    (out,) = call(
        final_kernel,
        [((4, TOK, 256), BF)],
        (y, placed("c"), pay, other_core(pay), *w_out),
        [pltpu.VMEM((8, TOK, 128), F32)],
        smem=2,
    )
    own = exchange(out, "x")
    other = other_core(own)
    hbm = pl.BlockSpec(memory_space=pl.ANY)
    c = placed("c")
    whole = pl.pallas_call(
        place_own,
        out_shape=jax.ShapeDtypeStruct((TOK, DIM), BF),
        in_specs=[SM, VM],
        out_specs=hbm,
        scratch_shapes=[pltpu.SemaphoreType.DMA((4,))],
        name="begin",
    )(c, own)
    return pl.pallas_call(
        place_other,
        out_shape=jax.ShapeDtypeStruct((TOK, DIM), BF),
        in_specs=[SM, VM, hbm],
        out_specs=hbm,
        scratch_shapes=[pltpu.SemaphoreType.DMA((4,))],
        input_output_aliases={2: 0},
        name="place",
    )(c, other, whole)


def solution(mesh):
    finer = Mesh(mesh.devices.reshape(4, 2, 2, 4, 4, 2), (*SP, *TP))
    return jax.shard_map(
        layer,
        mesh=finer,
        in_specs=(
            P(SP, None),
            P(),
            P(SP, TP),
            P(SP, TP),
            P(SP, TP),
            P(SP, TP),
            P(SP, TP),
            P(TP),
            P(),
            P(None, TP),
            P(TP),
            P(),
            P(None, TP),
            P(SP, TP),
            P(SP, TP),
            P(TP),
            P(None, TP),
            P(TP),
            P(SP, TP),
            P(SP, TP),
        ),
        out_specs=P(SP, None),
        check_vma=False,
    )
```
